256 devices in a mesh: grp: 2 (over y), kv: 16 (over z), tp: 8 (over x, core).
Axes of the slice: x: 4, y: 2, z: 16, core: 2. Of those that a mesh axis runs over, the one named last changes fastest.
The devices are a block of a 4x16x16 slice.
Arguments:
- piece_tokens: bfloat16 [8192, 2048], P(('grp', 'kv')), parts along dimension 0, may hold values from -6 to 6
- dec_tokens: bfloat16 [128, 2048], P(('grp', 'kv')), parts along dimension 0, may hold values from -6 to 6
- norm_gain: float32 [2048], replicated, may hold values from 0.1 to 1.9
- query_weight: bfloat16 [2048, 1024], P(None, 'tp'), may hold values from -0.125 to 0.125
- key_weight: bfloat16 [2048, 1024], P(None, 'tp'), may hold values from -0.125 to 0.125
- value_weight: bfloat16 [2048, 1024], P(None, 'tp'), may hold values from -0.125 to 0.125
- forget_weight: bfloat16 [2048, 8], P(None, 'tp'), may hold values from -0.125 to 0.125
- forget_bias: float32 [8], P('tp'), may hold values from 3 to 13
- out_weight: bfloat16 [1024, 2048], P(None, 'tp'), may hold values from -0.1875 to 0.1875
- cache_keys: bfloat16 [131072, 1024], P(('grp', 'kv'), 'tp'), parts along dimension 0, may hold values from -480 to 480
- cache_values: bfloat16 [131072, 1024], P(('grp', 'kv'), 'tp'), parts along dimension 0, may hold values from -6 to 6
- cache_gates: float32 [8, 131072], P('tp', ('grp', 'kv')), parts along dimension 1, as said below
- dec_keys: bfloat16 [128, 2048, 1024], P(('grp', 'kv'), None, 'tp'), parts along dimension 0, may hold values from -480 to 480
- dec_values: bfloat16 [128, 2048, 1024], P(('grp', 'kv'), None, 'tp'), parts along dimension 0, may hold values from -6 to 6
- dec_gates: float32 [128, 8, 2048], P(('grp', 'kv'), 'tp'), parts along dimension 0, as said below
- dec_lengths: int32 [128], P(('grp', 'kv')), parts along dimension 0, may hold values from 1 to 2048, as said below
Outputs:
- piece_out: bfloat16 [8192, 2048], P(('grp', 'kv'), 'tp'), parts along dimension 0
- dec_out: bfloat16 [128, 2048], P(('grp', 'kv'), 'tp'), parts along dimension 0
- piece_keys: bfloat16 [8192, 1024], P(('grp', 'kv'), 'tp'), parts along dimension 0
- piece_values: bfloat16 [8192, 1024], P(('grp', 'kv'), 'tp'), parts along dimension 0
The draws below stay inside these ranges and needn't reach their ends.
There are 2 independent parts, one for each index of `grp`. The reference program is written for one: setup_inputs(seed, part) draws one part's arguments, and reference() takes and returns one part's arrays. A program takes and returns all parts, laid end to end along the dimension named above; an argument that names none is the same for every part. Nothing has to cross between parts.
Inputs may be any that keep to these rules, and one draw needn't show every extreme that they name: cache_gates never falls along positions and is 0 at the last cached position. dec_gates never falls along a sequence's live slots and is 0 at its last live slot and beyond. Slots 0 to dec_lengths[b] - 1 of sequence b are live; some sequence has exactly 2048.
All inputs are finite; a program needn't handle non-finite values.
Results may differ from the reference program's by a relative error of at most 0.015.
Values may be sent and summed in bfloat16 or wider, within the bound.
A program may use at most 64 MiB of HBM per device.

```python
import math
import jax
import jax.numpy as jnp
from jax import lax

D = 2048
HEADS = 8
HEAD_DIM = 128
PIECE_DEV = 256
CACHE_DEV = 4096
DLEN = 2048
WIDTH = 1024
PIECE = 4096
CACHE = 65536
DEC = 64
N_KV = 16


def head_slowness(key):
    order = jax.random.permutation(jax.random.fold_in(key, 3), HEADS)
    slow_heads = order < HEADS // 2
    return slow_heads


def live_lengths(key):
    base_length = jax.random.randint(jax.random.fold_in(key, 21), (DEC,), 1, DLEN + 1)
    shifts = jax.random.randint(jax.random.fold_in(key, 22), (DEC,), 0, 3)
    lengths = jnp.maximum(jnp.right_shift(base_length, shifts), 1)
    chosen = jax.random.randint(jax.random.fold_in(key, 23), (), 0, DEC)
    return jnp.where(jnp.arange(DEC) == chosen, DLEN, lengths).astype(jnp.int32)


def draw_forget_bias(key, part):
    slow_heads = head_slowness(key)
    slow_level = max(math.log(0.5 * PIECE), math.log(200.0))
    levels = jnp.where(slow_heads, slow_level, jnp.log(50.0))
    jitter = jax.random.uniform(jax.random.fold_in(key, 4), (HEADS,), jnp.float32, -0.3, 0.3)
    return (levels + jitter).astype(jnp.float32)


def draw_cache_gates(key, part):
    slow_heads = head_slowness(jax.random.fold_in(key, 5))
    levels = jnp.where(slow_heads, jnp.log(1.6 * (CACHE + PIECE)), jnp.log(50.0))
    noise = jax.random.normal(jax.random.fold_in(key, 6), (HEADS, CACHE), jnp.float32) * 0.7
    span_count = CACHE // CACHE_DEV
    factors = jnp.exp(jax.random.uniform(jax.random.fold_in(key, 7), (HEADS, span_count), jnp.float32, -0.7, 0.7))
    factors = jnp.repeat(factors, CACHE_DEV, axis=1)
    rates = jnp.exp(-levels[:, None] - noise) * factors
    suffix = jnp.cumsum(rates[:, ::-1], axis=1)[:, ::-1] - rates
    return (-suffix).astype(jnp.float32)


def draw_dec_gates(key, part):
    slow_heads = head_slowness(jax.random.fold_in(key, 8))
    levels = jnp.where(slow_heads, jnp.log(1.6 * DLEN), jnp.log(50.0))
    noise = jax.random.normal(jax.random.fold_in(key, 9), (DEC, HEADS, DLEN), jnp.float32) * 0.7
    factors = jnp.exp(jax.random.uniform(jax.random.fold_in(key, 10), (DEC, HEADS, 1), jnp.float32, -0.7, 0.7))
    lengths = live_lengths(key)
    live_slots = jnp.arange(DLEN)[None, None, :] < lengths[:, None, None]
    rates = jnp.where(live_slots, jnp.exp(-levels[None, :, None] - noise) * factors, 0.0)
    suffix = jnp.cumsum(rates[:, :, ::-1], axis=2)[:, :, ::-1] - rates
    return (-suffix).astype(jnp.float32)


def draw_dec_lengths(key, part):
    return live_lengths(key)


def draw_cache_keys(key, part):
    values = jnp.clip(jax.random.normal(jax.random.fold_in(key, 11), (CACHE, WIDTH), jnp.float32), -6.0, 6.0)
    return values.astype(jnp.bfloat16)


def draw_dec_keys(key, part):
    values = jnp.clip(jax.random.normal(jax.random.fold_in(key, 13), (DEC, DLEN, WIDTH), jnp.float32), -6.0, 6.0)
    return values.astype(jnp.bfloat16)


def steps_of(own_key, shape, shards, least, largest):
    loudness, own = 1.0, jax.random.fold_in(own_key, 6)
    for position, blocks in shards:
        heights = jnp.exp(jax.random.uniform(jax.random.fold_in(own, position), (blocks,), jnp.float32, least / len(shards), largest / len(shards)))
        loudness = loudness * jnp.repeat(heights, shape[position] // blocks).reshape([-1 if axis == position else 1 for axis in range(len(shape))])
    return loudness


def scatter_about(rng, dims, width, bound, shards=(), held_as=jnp.bfloat16):
    values = width * jax.random.normal(rng, dims, jnp.float32)
    if shards:
        values = values * steps_of(rng, dims, shards, -0.22, 0.18)
    return jnp.clip(values, -bound, bound).astype(held_as)


def setup_inputs(seed: int = 0, part: int = 0) -> dict:
    key_list = jax.random.split(jax.random.key(seed), 17)
    part_keys = jax.random.split(jax.random.fold_in(key_list[16], part), 17)
    return {
        "piece_tokens": scatter_about(part_keys[0], (PIECE, D), 1.0, 6.0, ((0, 16),)),
        "dec_tokens": scatter_about(part_keys[1], (DEC, D), 1.0, 6.0, ((0, 16),)),
        "norm_gain": jnp.clip(1.0 + 0.18 * jax.random.normal(key_list[2], (D,), jnp.float32), 0.1, 1.9),
        "query_weight": scatter_about(key_list[3], (D, WIDTH), D ** -0.5, 0.125, ((1, 8),)),
        "key_weight": scatter_about(key_list[4], (D, WIDTH), D ** -0.5, 0.125, ((1, 8),)),
        "value_weight": scatter_about(key_list[5], (D, WIDTH), D ** -0.5, 0.125, ((1, 8),)),
        "forget_weight": scatter_about(key_list[6], (D, HEADS), D ** -0.5, 0.125, ((1, 8),)),
        "forget_bias": draw_forget_bias(jax.random.fold_in(key_list[16], 71), part),
        "out_weight": scatter_about(key_list[8], (WIDTH, D), WIDTH ** -0.5, 0.1875, ((1, 8),)),
        "cache_keys": draw_cache_keys(jax.random.fold_in(jax.random.fold_in(key_list[16], part), 71), part),
        "cache_values": scatter_about(part_keys[10], (CACHE, WIDTH), 1.0, 6.0, ((0, 16), (1, 8))),
        "cache_gates": draw_cache_gates(jax.random.fold_in(jax.random.fold_in(key_list[16], part), 71), part),
        "dec_keys": draw_dec_keys(jax.random.fold_in(jax.random.fold_in(key_list[16], part), 71), part),
        "dec_values": scatter_about(part_keys[13], (DEC, DLEN, WIDTH), 1.0, 6.0, ((0, 16), (2, 8))),
        "dec_gates": draw_dec_gates(jax.random.fold_in(jax.random.fold_in(key_list[16], part), 71), part),
        "dec_lengths": draw_dec_lengths(jax.random.fold_in(jax.random.fold_in(key_list[16], part), 71), part),
    }


norm_eps = 1e-05

def rms_norm(tokens, norm_gain):
    values = tokens.astype(jnp.float32)
    factor = lax.rsqrt(lax.optimization_barrier(jnp.mean(values * values, axis=-1, keepdims=True)) + norm_eps)
    return (values * factor * norm_gain.astype(jnp.float32)).astype(jnp.bfloat16)

def project(tokens, norm_gain, query_weight, key_weight, value_weight, forget_weight, forget_bias):
    normed = rms_norm(tokens, norm_gain)
    queries = jnp.dot(normed, query_weight, preferred_element_type=jnp.float32).astype(jnp.bfloat16)
    key_rows = jnp.dot(normed, key_weight, preferred_element_type=jnp.float32).astype(jnp.bfloat16)
    value_rows = jnp.dot(normed, value_weight, preferred_element_type=jnp.float32).astype(jnp.bfloat16)
    log_gates = jax.nn.log_sigmoid(jnp.dot(normed, forget_weight, preferred_element_type=jnp.float32) + forget_bias.astype(jnp.float32))
    return (queries, key_rows, value_rows, log_gates)

def reference(piece_tokens, dec_tokens, norm_gain, query_weight, key_weight, value_weight, forget_weight, forget_bias, out_weight, cache_keys, cache_values, cache_gates, dec_keys, dec_values, dec_gates, dec_lengths):
    piece_queries, piece_keys, piece_values, piece_gates = project(piece_tokens, norm_gain, query_weight, key_weight, value_weight, forget_weight, forget_bias)
    dec_queries, dec_new_keys, dec_new_values, dec_gate_now = project(dec_tokens, norm_gain, query_weight, key_weight, value_weight, forget_weight, forget_bias)
    score_scale = HEAD_DIM ** (-0.5)
    prefix = jnp.cumsum(piece_gates, axis=0)
    piece_bias = -prefix.T
    block_rows = math.gcd(PIECE, 1024)
    block_count = PIECE // block_rows
    query_blocks = piece_queries.astype(jnp.float32).reshape(block_count, block_rows, HEADS, HEAD_DIM)
    block_starts = jnp.arange(block_count, dtype=jnp.int32) * block_rows

    def shard_keys(shard_number):
        cache_first = (shard_number * CACHE_DEV).astype(jnp.int32)
        piece_first = (shard_number * PIECE_DEV).astype(jnp.int32)
        key_rows = jnp.concatenate([lax.dynamic_slice_in_dim(cache_keys, cache_first, CACHE_DEV, 0), lax.dynamic_slice_in_dim(piece_keys, piece_first, PIECE_DEV, 0)], 0)
        value_rows = jnp.concatenate([lax.dynamic_slice_in_dim(cache_values, cache_first, CACHE_DEV, 0), lax.dynamic_slice_in_dim(piece_values, piece_first, PIECE_DEV, 0)], 0)
        key_bias = jnp.concatenate([lax.dynamic_slice_in_dim(cache_gates, cache_first, CACHE_DEV, 1), lax.dynamic_slice_in_dim(piece_bias, piece_first, PIECE_DEV, 1)], 1)
        key_order = jnp.concatenate([jnp.full((CACHE_DEV,), -1, jnp.int32), piece_first + jnp.arange(PIECE_DEV, dtype=jnp.int32)])
        key_rows = key_rows.astype(jnp.float32).reshape(-1, HEADS, HEAD_DIM)
        value_rows = value_rows.astype(jnp.float32).reshape(-1, HEADS, HEAD_DIM)
        return (key_rows, value_rows, key_bias, key_order)

    def block_scores(key_rows, key_bias, key_order, query_block, first_row):
        scores = jnp.einsum('qhd,khd->hqk', query_block, key_rows) * score_scale + key_bias[:, None, :]
        query_order = first_row + jnp.arange(block_rows, dtype=jnp.int32)
        visible = key_order[None, :] <= query_order[:, None]
        return jnp.where(visible[None], scores, -jnp.inf)

    def shard_terms(shard_number):
        key_rows, value_rows, key_bias, key_order = shard_keys(shard_number)

        def one_block(inputs):
            query_block, first_row = inputs
            scores = block_scores(key_rows, key_bias, key_order, query_block, first_row)
            local_max = lax.optimization_barrier(jnp.max(scores, axis=-1))
            weights_exp = jnp.exp(scores - local_max[:, :, None])
            rounded = lax.optimization_barrier(weights_exp.astype(jnp.bfloat16)).astype(jnp.float32)
            numerator = jnp.einsum('hqk,khd->qhd', rounded, value_rows).astype(jnp.bfloat16)
            return (numerator, lax.optimization_barrier(jnp.sum(weights_exp, axis=-1)), local_max)
        return lax.map(one_block, (query_blocks, block_starts))
    shard_numbers = jnp.arange(N_KV, dtype=jnp.int32)
    numerators, denominators, local_maxima = lax.map(shard_terms, shard_numbers)
    maxima = lax.optimization_barrier(jnp.max(local_maxima, axis=0))
    factors = jnp.exp(local_maxima - maxima[None])
    factor_rows = jnp.transpose(factors, (0, 1, 3, 2))[..., None]
    scaled = (numerators.astype(jnp.float32) * factor_rows).astype(jnp.bfloat16)
    scaled = lax.optimization_barrier(scaled).astype(jnp.float32)
    numer_sum = lax.optimization_barrier(jnp.sum(scaled, axis=0))
    denom_sum = jnp.transpose(lax.optimization_barrier(jnp.sum(denominators * factors, axis=0)), (0, 2, 1))
    piece_attention = (numer_sum / denom_sum[..., None]).astype(jnp.bfloat16).reshape(PIECE, HEADS * HEAD_DIM)

    def one_sequence(inputs):
        query_row, new_key, new_value, gate_now, seq_keys, seq_values, seq_gates, seq_length = inputs
        query_heads = query_row.astype(jnp.float32).reshape(HEADS, HEAD_DIM)
        key_heads = seq_keys.astype(jnp.float32).reshape(DLEN, HEADS, HEAD_DIM)
        value_heads = seq_values.astype(jnp.float32).reshape(DLEN, HEADS, HEAD_DIM)
        cached = jnp.einsum('hd,khd->hk', query_heads, key_heads) * score_scale + seq_gates + gate_now[:, None]
        live_slots = jnp.arange(DLEN, dtype=jnp.int32) < seq_length
        cached = jnp.where(live_slots[None, :], cached, -jnp.inf)
        own_score = lax.optimization_barrier(jnp.sum(query_heads * new_key.astype(jnp.float32).reshape(HEADS, HEAD_DIM), axis=-1)) * score_scale
        row_top = jnp.maximum(lax.optimization_barrier(jnp.max(cached, axis=-1)), own_score)
        cached_exp = jnp.exp(cached - row_top[:, None])
        own_exp = jnp.exp(own_score - row_top)
        whole_sum = lax.optimization_barrier(jnp.sum(cached_exp, axis=-1)) + own_exp
        cached_weights = (cached_exp / whole_sum[:, None]).astype(jnp.bfloat16).astype(jnp.float32)
        own_weights = (own_exp / whole_sum).astype(jnp.bfloat16).astype(jnp.float32)
        mixed = jnp.einsum('hk,khd->hd', cached_weights, value_heads) + own_weights[:, None] * new_value.astype(jnp.float32).reshape(HEADS, HEAD_DIM)
        return mixed.astype(jnp.bfloat16).reshape(HEADS * HEAD_DIM)
    dec_attention = lax.map(one_sequence, (dec_queries, dec_new_keys, dec_new_values, dec_gate_now, dec_keys, dec_values, dec_gates, dec_lengths))
    piece_out = jnp.dot(piece_attention, out_weight, preferred_element_type=jnp.float32).astype(jnp.bfloat16)
    dec_out = jnp.dot(dec_attention, out_weight, preferred_element_type=jnp.float32).astype(jnp.bfloat16)
    return (piece_out, dec_out, piece_keys, piece_values)
```

```python
import functools
import math

import jax
import jax.numpy as jnp
from jax import lax
from jax.experimental import pallas as pl
from jax.experimental.pallas import tpu as pltpu
from jax.sharding import PartitionSpec as P

norm_eps = 1e-05
bf16 = jnp.bfloat16
f32 = jnp.float32
MESH = pl.DeviceIdType.MESH
NEG = -1e30
LANES = 128
KEY_CHUNK = 2048


def dot(a, b):
    return jnp.dot(a, b, preferred_element_type=f32)


def three_parts(x):
    high = x.astype(bf16)
    rest = x - high.astype(f32)
    middle = rest.astype(bf16)
    low = (rest - middle.astype(f32)).astype(bf16)
    return high, middle, low


def row_max(x, rows=64):
    n = x.shape[0]
    if n > rows:
        x = jnp.max(x.reshape(n // rows, rows, x.shape[1]), axis=0)
    return jnp.max(x, axis=0, keepdims=True)


def kernel(
    tok_hbm,
    dtok_ref,
    gain_ref,
    wq_hbm,
    wk_hbm,
    wv_hbm,
    fw_ref,
    fb_ref,
    ow_hbm,
    ck_hbm,
    cv_hbm,
    cg_ref,
    dk_hbm,
    dv_hbm,
    dg_ref,
    dl_ref,
    po_ref,
    do_ref,
    pk_ref,
    pv_ref,
    tok,
    wq,
    wk,
    wv,
    ow,
    cv,
    dk,
    dv,
    normed,
    kaug,
    v_t,
    ones_rows,
    qbuf,
    acc_in,
    ml_in,
    acc_out,
    ml_out,
    unit_acc,
    unit_ml,
    own_acc,
    own_ml,
    totals,
    att,
    datt,
    local_sem,
    q_send,
    q_recv,
    acc_send,
    acc_recv,
    ml_send,
    ml_recv,
    tot_send,
    tot_recv,
    att_send,
    att_recv,
    datt_send,
    datt_recv,
    *,
    chains,
):
    n = lax.axis_size("kv")
    heads = lax.axis_size("tp")
    me = lax.axis_index("kv")
    my_tp = lax.axis_index("tp")
    right = lax.rem(me + 1, n)
    left = lax.rem(me + n - 1, n)
    piece, width = tok.shape
    half = piece // 2
    depth = wq.shape[1]
    cache = cv.shape[0]
    decs, span = dk.shape[0], dk.shape[1]
    length = n // chains
    scale = depth ** (-0.5)
    root = depth**0.5
    c2 = scale * math.log2(math.e)

    def load(i, src, dst):
        return pltpu.make_async_copy(src, dst, local_sem.at[i])

    loads = [
        load(0, tok_hbm, tok),
        load(1, wq_hbm, wq),
        load(2, wk_hbm, wk),
        load(3, wv_hbm, wv),
        load(4, cv_hbm, cv),
        load(5, ck_hbm, kaug.at[pl.ds(0, cache), pl.ds(0, depth)]),
        load(6, dk_hbm, dk),
        load(7, dv_hbm, dv),
        load(8, ow_hbm, ow),
    ]
    barrier = pltpu.get_barrier_semaphore()
    for d in range(1, n):
        pl.semaphore_signal(
            barrier, inc=1, device_id={"kv": lax.rem(me + d, n)}, device_id_type=MESH
        )
    for d in range(1, heads):
        pl.semaphore_signal(
            barrier, inc=1, device_id={"tp": lax.rem(my_tp + d, heads)}, device_id_type=MESH
        )
    for c in loads:
        c.start()

    def total_copy(d):
        return pltpu.make_async_remote_copy(
            src_ref=totals.at[0],
            dst_ref=totals.at[d],
            send_sem=tot_send.at[d],
            recv_sem=tot_recv.at[d],
            device_id={"kv": lax.rem(me + d, n)},
            device_id_type=MESH,
        )

    def q_copy(src, dst, side, target):
        return pltpu.make_async_remote_copy(
            src_ref=qbuf.at[src, side],
            dst_ref=qbuf.at[dst, side],
            send_sem=q_send.at[dst, side],
            recv_sem=q_recv.at[dst, side],
            device_id={"kv": target},
            device_id_type=MESH,
        )

    def acc_copies(src, dst, side, target):
        return (
            pltpu.make_async_remote_copy(
                src_ref=acc_out.at[src, side],
                dst_ref=acc_in.at[dst, side],
                send_sem=acc_send.at[src, side],
                recv_sem=acc_recv.at[dst, side],
                device_id={"kv": target},
                device_id_type=MESH,
            ),
            pltpu.make_async_remote_copy(
                src_ref=ml_out.at[src, side],
                dst_ref=ml_in.at[dst, side],
                send_sem=ml_send.at[src, side],
                recv_sem=ml_recv.at[dst, side],
                device_id={"kv": target},
                device_id_type=MESH,
            ),
        )

    def att_copy(d, src_slot, dst_slot):
        return pltpu.make_async_remote_copy(
            src_ref=att.at[src_slot],
            dst_ref=att.at[dst_slot],
            send_sem=att_send.at[d],
            recv_sem=att_recv.at[d],
            device_id={"tp": lax.rem(my_tp + d, heads)},
            device_id_type=MESH,
        )

    def datt_copy(d, src_slot, dst_slot):
        return pltpu.make_async_remote_copy(
            src_ref=datt.at[src_slot],
            dst_ref=datt.at[dst_slot],
            send_sem=datt_send.at[d],
            recv_sem=datt_recv.at[d],
            device_id={"tp": lax.rem(my_tp + d, heads)},
            device_id_type=MESH,
        )

    gain = gain_ref[...]
    rows_at_once = 64

    def norm_rows(x):
        x = x.astype(f32)
        factor = lax.rsqrt(jnp.mean(x * x, axis=-1, keepdims=True) + norm_eps)
        return (x * factor * gain).astype(bf16)

    loads[0].wait()
    for r in range(0, piece, rows_at_once):
        normed[r : r + rows_at_once, :] = norm_rows(tok[r : r + rows_at_once, :])
    drows = norm_rows(dtok_ref[...])
    normed[piece:, :] = jnp.concatenate(
        [drows, jnp.zeros((normed.shape[0] - piece - decs, width), bf16)], axis=0
    )
    loads[1].wait()
    queries = dot(normed[...], wq[...]).astype(bf16)
    q_t = queries[:piece, :].T
    for side in range(2):
        qbuf[0, side] = q_t[:, side * half : (side + 1) * half]
    gate_in = dot(normed[...], fw_ref[...])[:, 0:1] + fb_ref[...]
    log_gates = jnp.minimum(gate_in, 0.0) - jnp.log1p(jnp.exp(-jnp.abs(gate_in)))
    piece_gates = log_gates[:piece]
    lane = lax.broadcasted_iota(jnp.int32, (piece, LANES), 1)
    hi, mid, lo = three_parts(piece_gates)
    zero = jnp.zeros((), f32)

    def columns(a, b, c, rows):
        at = lax.broadcasted_iota(jnp.int32, (rows, LANES), 1)
        out = jnp.where(at == 0, a.astype(f32), zero)
        out = jnp.where(at == 1, b.astype(f32), out)
        out = jnp.where(at == 2, c.astype(f32), out)
        return out.astype(bf16)

    below = (
        lax.broadcasted_iota(jnp.int32, (piece, piece), 1)
        <= lax.broadcasted_iota(jnp.int32, (piece, piece), 0)
    ).astype(f32)
    running = dot(below.astype(bf16), columns(hi, mid, lo, piece))
    running = running[:, 0:1] + running[:, 1:2] + running[:, 2:3]
    totals[0] = jnp.broadcast_to(running[piece - 1 : piece, :], (8, LANES))

    pl.semaphore_wait(barrier, n - 1 + heads - 1)
    for side, target in ((0, right), (1, left)):
        q_copy(0, 1, side, target).start()
    for d in range(1, n):
        total_copy(d).start()
    for c in range(1, chains):
        o = 1 + c * length
        q_copy(0, o, 0, lax.rem(me + o, n)).start()
        q_copy(0, o, 1, lax.rem(me - o + n, n)).start()

    loads[2].wait()
    key_rows = dot(normed[...], wk[...]).astype(bf16)
    pk_ref[...] = key_rows[:piece]
    kaug[cache:, :depth] = key_rows[:piece]
    loads[3].wait()
    value_rows = dot(normed[...], wv[...]).astype(bf16)
    pv_ref[...] = value_rows[:piece]
    v_t[:depth, cache:] = value_rows[:piece].T
    v_t[depth:, :] = jnp.ones((v_t.shape[0] - depth, v_t.shape[1]), bf16)
    kaug[cache:, depth:] = columns(*three_parts(-running * root), piece)
    at_row = lax.broadcasted_iota(jnp.int32, (LANES, 2 * piece), 0)
    ones_rows[...] = jnp.where(at_row < 3, 1.0, 0.0)[:, :piece].astype(bf16)
    for r in range(0, cache, 512):
        gates = jnp.maximum(cg_ref[:, r : r + 512], NEG) * root
        a, b, c = three_parts(gates)
        at = lax.broadcasted_iota(jnp.int32, (LANES, 512), 0)
        rows = jnp.where(at == 0, a.astype(f32), zero)
        rows = jnp.where(at == 1, b.astype(f32), rows)
        rows = jnp.where(at == 2, c.astype(f32), rows)
        kaug[r : r + 512, depth:] = rows.astype(bf16).T
    loads[4].wait()
    for r in range(0, cache, 512):
        v_t[:depth, r : r + 512] = cv[r : r + 512, :].T
    loads[5].wait()

    loads[6].wait()
    dec_q = queries[piece:, :]
    dec_k = key_rows[piece:, :]
    dec_v = value_rows[piece:, :]
    scores = []
    for b in range(decs):
        s = lax.dot_general(
            dec_q, dk[b], (((1,), (1,)), ((), ())), preferred_element_type=f32
        )
        scores.append(s[b : b + 1])
    cached = jnp.concatenate(scores, axis=0) * scale + dg_ref[...] + log_gates[piece : piece + decs]
    slot = lax.broadcasted_iota(jnp.int32, (decs, span), 1)
    cached = jnp.where(slot < dl_ref[...], cached, -jnp.inf)
    own_score = (
        jnp.sum(dec_q.astype(f32) * dec_k.astype(f32), axis=-1, keepdims=True)[:decs] * scale
    )
    top = jnp.maximum(jnp.max(cached, axis=-1, keepdims=True), own_score)
    cached_exp = jnp.exp(cached - top)
    own_exp = jnp.exp(own_score - top)
    whole = jnp.sum(cached_exp, axis=-1, keepdims=True) + own_exp
    weights = (cached_exp / whole).astype(bf16)
    own_weight = (own_exp / whole).astype(bf16).astype(f32)
    weights = jnp.concatenate(
        [weights, jnp.zeros((dec_q.shape[0] - decs, span), bf16)], axis=0
    )
    loads[7].wait()
    mixed = [dot(weights, dv[b])[b : b + 1] for b in range(decs)]
    mixed = jnp.concatenate(mixed, axis=0) + own_weight * dec_v[:decs].astype(f32)
    datt[0] = jnp.concatenate(
        [mixed, jnp.zeros((dec_q.shape[0] - decs, depth), f32)], axis=0
    ).astype(bf16)
    for d in range(1, heads):
        datt_copy(d, 0, d).start()

    chunks = [(cache, cache + piece)] + [
        (k, k + KEY_CHUNK) for k in range(0, cache, KEY_CHUNK)
    ]
    lane_row = lax.broadcasted_iota(jnp.int32, (1, piece), 1)

    def local_terms(o, offset):
        block_a = lax.rem(me - o + n, n)
        block_b = lax.rem(me + o, n)
        slot_o = lax.rem(o, n)
        q_block = jnp.concatenate([qbuf[slot_o, 0], qbuf[slot_o, 1]], axis=1)
        q_block = jnp.concatenate([q_block, ones_rows[...]], axis=0)
        query_order = jnp.where(lane_row < half, block_a, block_b) * piece + lane_row
        s = dot(kaug[chunks[0][0] : chunks[0][1], :], q_block)
        terms = []
        for i, (k0, k1) in enumerate(chunks):
            if i == 0:
                key_order = me * piece + lax.broadcasted_iota(jnp.int32, (piece, 1), 0)
                s = jnp.where(key_order <= query_order, s, NEG)
            top_i = row_max(s)
            if i + 1 < len(chunks):
                s_next = dot(kaug[chunks[i + 1][0] : chunks[i + 1][1], :], q_block)
            weights_i = jnp.exp2((s - top_i) * c2).astype(bf16)
            sums = dot(v_t[:, k0:k1], weights_i)
            terms.append((sums, top_i - offset * root if i == 0 else top_i))
            s = s_next
        top_all = functools.reduce(jnp.maximum, [t for _, t in terms])
        total = None
        for sums, t in terms:
            part = sums * jnp.exp2((t - top_all) * c2)
            total = part if total is None else total + part
        return total[:depth], top_all, total[depth : depth + 1]

    def ml_rows(m, l):
        return jnp.concatenate([m, l, jnp.zeros((6, m.shape[1]), f32)], axis=0)

    def merge(acc_a, m_a, l_a, acc_b, m_b, l_b):
        m = jnp.maximum(m_a, m_b)
        f_a = jnp.exp2((m_a - m) * c2)
        f_b = jnp.exp2((m_b - m) * c2)
        return acc_a * f_a + acc_b * f_b, m, l_a * f_a + l_b * f_b

    for d in range(1, n):
        total_copy(d).wait_recv()
    offset = jnp.zeros((1, LANES), f32)
    for d in range(1, n):
        offset = offset + jnp.where(d <= me, totals[d][0:1, :], 0.0)
    offset = jnp.concatenate([offset] * (piece // LANES), axis=1)

    skew = 2 if chains > 1 else 0
    paired = length - skew if chains > 1 else 0

    def order(u):
        if chains == 1:
            return jnp.where(u == 0, n, u)
        k = u - 1 - skew
        middle = jnp.where(
            lax.rem(k, 2) == 0, 1 + skew + k // 2, 1 + length + k // 2
        )
        o = jnp.where(u < 1 + skew, u, jnp.where(k < 2 * paired, middle, u))
        return jnp.where(u == 0, n, o)

    def unit(u, carry):
        o = order(u)
        starts = lax.rem(o, length) == 1
        ends = lax.rem(o, length) == 0

        @pl.when(o < n)
        def _():
            for side in range(2):
                q_copy(0, o, side, right).wait_recv()

        @pl.when(jnp.logical_and(jnp.logical_not(ends), o < n - 1))
        def _():
            for side, target in ((0, right), (1, left)):
                q_copy(o, o + 1, side, target).start()

        acc, m, l = local_terms(o, offset)
        unit_acc[...] = acc
        unit_ml[...] = ml_rows(m, l)

        @pl.when(o == n)
        def _():
            own_acc[...] = unit_acc[...]
            own_ml[...] = unit_ml[...]

        @pl.when(o < n)
        def _():
            @pl.when(starts)
            def _():
                for side in range(2):
                    acc_in[o, side] = jnp.zeros((depth, half), bf16)
                    ml_in[o, side] = jnp.where(
                        lax.broadcasted_iota(jnp.int32, (8, half), 0) == 0, NEG, 0.0
                    )

            @pl.when(jnp.logical_not(starts))
            def _():
                for side in range(2):
                    for c in acc_copies(0, o, side, right):
                        c.wait_recv()

            for side in range(2):
                at = slice(side * half, (side + 1) * half)
                ml = ml_in[o, side]
                a, mm, ll = merge(
                    unit_acc[:, at],
                    unit_ml[0:1, at],
                    unit_ml[1:2, at],
                    acc_in[o, side].astype(f32),
                    ml[0:1],
                    ml[1:2],
                )
                acc_out[o, side] = a.astype(bf16)
                ml_out[o, side] = ml_rows(mm, ll)
            goes = jnp.where(ends, o, 1)
            dst = jnp.where(ends, n + o // length, o + 1)
            for c in acc_copies(o, dst, 0, lax.rem(me + jnp.where(ends, n - goes, 1), n)):
                c.start()
            for c in acc_copies(o, dst, 1, lax.rem(me + jnp.where(ends, goes, n - 1), n)):
                c.start()

        return carry

    lax.fori_loop(0, n, unit, 0)

    halves = []
    for side in range(2):
        at = slice(side * half, (side + 1) * half)
        state = (own_acc[:, at], own_ml[0:1, at], own_ml[1:2, at])
        for slot_i in [n + c for c in range(1, chains)] + [n]:
            for c in acc_copies(0, slot_i, side, right):
                c.wait_recv()
            ml = ml_in[slot_i, side]
            state = merge(*state, acc_in[slot_i, side].astype(f32), ml[0:1], ml[1:2])
        halves.append((state[0] / state[2]).astype(bf16))
    att[0] = jnp.concatenate(halves, axis=1).T
    for d in range(1, heads):
        att_copy(d, 0, d).start()

    def weight_of(d):
        head = lax.rem(my_tp - d + heads, heads)
        return ow[pl.ds(pl.multiple_of(head * depth, depth), depth), :]

    loads[8].wait()
    dec_sum = dot(datt[0], weight_of(0))
    for d in range(1, heads):
        datt_copy(d, 0, d).wait_recv()
        dec_sum = dec_sum + dot(datt[d], weight_of(d))
    do_ref[...] = dec_sum[:decs].astype(bf16)
    out = dot(att[0], weight_of(0))
    for d in range(1, heads):
        att_copy(d, 0, d).wait_recv()
        out = out + dot(att[d], weight_of(d))
    po_ref[...] = out.astype(bf16)

    for d in range(1, n):
        total_copy(d).wait_send()
    for d in range(1, heads):
        att_copy(d, 0, d).wait_send()
        datt_copy(d, 0, d).wait_send()

    def sent(o, carry):
        for side in range(2):
            q_copy(0, o, side, right).wait_send()
            for c in acc_copies(o, n, side, right):
                c.wait_send()
        return carry

    lax.fori_loop(1, n, sent, 0)


def shards(
    piece_tokens,
    dec_tokens,
    norm_gain,
    query_weight,
    key_weight,
    value_weight,
    forget_weight,
    forget_bias,
    out_weight,
    cache_keys,
    cache_values,
    cache_gates,
    dec_keys,
    dec_values,
    dec_gates,
    dec_lengths,
):
    n = lax.axis_size("kv")
    heads = lax.axis_size("tp")
    piece, width = piece_tokens.shape
    decs, span = dec_tokens.shape[0], dec_keys.shape[1]
    depth = query_weight.shape[1]
    cache = cache_keys.shape[0]
    out_columns = out_weight.shape[1]
    half = piece // 2
    chains = 2
    rows = piece + 16
    vmem = pl.BlockSpec(memory_space=pltpu.VMEM)
    hbm = pl.BlockSpec(memory_space=pl.ANY)
    dma = pltpu.SemaphoreType.DMA
    slots = n + chains
    gate_weight = jnp.concatenate(
        [forget_weight, jnp.zeros((width, LANES - forget_weight.shape[1]), bf16)], axis=1
    )
    return pl.pallas_call(
        functools.partial(kernel, chains=chains),
        out_shape=(
            jax.ShapeDtypeStruct((piece, out_columns), bf16),
            jax.ShapeDtypeStruct((decs, out_columns), bf16),
            jax.ShapeDtypeStruct((piece, depth), bf16),
            jax.ShapeDtypeStruct((piece, depth), bf16),
        ),
        in_specs=[hbm, vmem, vmem, hbm, hbm, hbm, vmem, vmem, hbm, hbm, hbm, vmem, hbm, hbm, vmem, vmem],
        out_specs=(vmem, vmem, vmem, vmem),
        scratch_shapes=[
            pltpu.VMEM((piece, width), bf16),
            pltpu.VMEM((width, depth), bf16),
            pltpu.VMEM((width, depth), bf16),
            pltpu.VMEM((width, depth), bf16),
            pltpu.VMEM(out_weight.shape, bf16),
            pltpu.VMEM((cache, depth), bf16),
            pltpu.VMEM(dec_keys.shape, bf16),
            pltpu.VMEM(dec_values.shape, bf16),
            pltpu.VMEM((rows, width), bf16),
            pltpu.VMEM((cache + piece, depth + LANES), bf16),
            pltpu.VMEM((depth + 16, cache + piece), bf16),
            pltpu.VMEM((LANES, piece), bf16),
            pltpu.VMEM((n, 2, depth, half), bf16),
            pltpu.VMEM((slots, 2, depth, half), bf16),
            pltpu.VMEM((slots, 2, 8, half), f32),
            pltpu.VMEM((n, 2, depth, half), bf16),
            pltpu.VMEM((n, 2, 8, half), f32),
            pltpu.VMEM((depth, piece), f32),
            pltpu.VMEM((8, piece), f32),
            pltpu.VMEM((depth, piece), f32),
            pltpu.VMEM((8, piece), f32),
            pltpu.VMEM((n, 8, LANES), f32),
            pltpu.VMEM((heads, piece, depth), bf16),
            pltpu.VMEM((heads, 16, depth), bf16),
            dma((9,)),
            dma((n, 2)),
            dma((n, 2)),
            dma((n, 2)),
            dma((slots, 2)),
            dma((n, 2)),
            dma((slots, 2)),
            dma((n,)),
            dma((n,)),
            dma((heads,)),
            dma((heads,)),
            dma((heads,)),
            dma((heads,)),
        ],
        compiler_params=pltpu.CompilerParams(
            collective_id=0, has_side_effects=True, vmem_limit_bytes=60 * 2**20
        ),
    )(
        piece_tokens,
        dec_tokens,
        norm_gain.reshape(1, width),
        query_weight,
        key_weight,
        value_weight,
        gate_weight,
        forget_bias.reshape(1, 1),
        out_weight,
        cache_keys,
        cache_values,
        cache_gates,
        dec_keys,
        dec_values,
        dec_gates.reshape(decs, span),
        dec_lengths.reshape(decs, 1),
    )


def solution(mesh):
    return jax.shard_map(
        shards,
        mesh=mesh,
        in_specs=(
            P(("grp", "kv"), None),
            P(("grp", "kv"), None),
            P(),
            P(None, "tp"),
            P(None, "tp"),
            P(None, "tp"),
            P(None, "tp"),
            P("tp"),
            P(None, "tp"),
            P(("grp", "kv"), "tp"),
            P(("grp", "kv"), "tp"),
            P("tp", ("grp", "kv")),
            P(("grp", "kv"), None, "tp"),
            P(("grp", "kv"), None, "tp"),
            P(("grp", "kv"), "tp", None),
            P(("grp", "kv")),
        ),
        out_specs=(
            P(("grp", "kv"), "tp"),
            P(("grp", "kv"), "tp"),
            P(("grp", "kv"), "tp"),
            P(("grp", "kv"), "tp"),
        ),
        check_vma=False,
    )
```

```python
import functools
import math

import jax
import jax.numpy as jnp
from jax import lax
from jax.experimental import pallas as pl
from jax.experimental.pallas import tpu as pltpu
from jax.sharding import PartitionSpec as P

norm_eps = 1e-05
bf16 = jnp.bfloat16
f32 = jnp.float32
MESH = pl.DeviceIdType.MESH
NEG = -1e30
LANES = 128
KEY_CHUNK = 2048


def dot(a, b):
    return jnp.dot(a, b, preferred_element_type=f32)


def three_parts(x):
    high = x.astype(bf16)
    rest = x - high.astype(f32)
    middle = rest.astype(bf16)
    low = (rest - middle.astype(f32)).astype(bf16)
    return high, middle, low


def row_max(x, rows=64):
    n = x.shape[0]
    if n > rows:
        x = jnp.max(x.reshape(n // rows, rows, x.shape[1]), axis=0)
    return jnp.max(x, axis=0, keepdims=True)


def kernel(
    tok_hbm,
    dtok_ref,
    gain_ref,
    wq_hbm,
    wk_hbm,
    wv_hbm,
    fw_ref,
    fb_ref,
    ow_hbm,
    ck_hbm,
    cv_hbm,
    cg_ref,
    dk_hbm,
    dv_hbm,
    dg_ref,
    dl_ref,
    po_ref,
    do_ref,
    pk_ref,
    pv_ref,
    tok,
    wq,
    wk,
    wv,
    ow,
    cv,
    dk,
    dv,
    normed,
    kaug,
    v_t,
    ones_rows,
    qbuf,
    acc_in,
    ml_in,
    acc_out,
    ml_out,
    unit_acc,
    unit_ml,
    own_acc,
    own_ml,
    totals,
    att,
    datt,
    dec_rows,
    dec_gate,
    local_sem,
    q_send,
    q_recv,
    acc_send,
    acc_recv,
    ml_send,
    ml_recv,
    tot_send,
    tot_recv,
    att_send,
    att_recv,
    datt_send,
    datt_recv,
    *,
    chains,
):
    n = lax.axis_size("kv")
    heads = lax.axis_size("tp")
    me = lax.axis_index("kv")
    my_tp = lax.axis_index("tp")
    right = lax.rem(me + 1, n)
    left = lax.rem(me + n - 1, n)
    piece, width = tok.shape
    half = piece // 2
    depth = wq.shape[1]
    cache = cv.shape[0]
    decs, span = dk.shape[0], dk.shape[1]
    length = n // chains
    scale = depth ** (-0.5)
    root = depth**0.5
    c2 = scale * math.log2(math.e)

    def load(i, src, dst):
        return pltpu.make_async_copy(src, dst, local_sem.at[i])

    loads = [
        load(0, tok_hbm, tok),
        load(1, wq_hbm, wq),
        load(2, wk_hbm, wk),
        load(3, wv_hbm, wv),
        load(4, cv_hbm, cv),
        load(5, ck_hbm, kaug.at[pl.ds(0, cache), pl.ds(0, depth)]),
        load(6, dk_hbm, dk),
        load(7, dv_hbm, dv),
        load(8, ow_hbm, ow),
    ]
    loads[0].start()
    loads[1].start()
    barrier = pltpu.get_barrier_semaphore()
    for d in range(1, n):
        pl.semaphore_signal(
            barrier, inc=1, device_id={"kv": lax.rem(me + d, n)}, device_id_type=MESH
        )
    for d in range(1, heads):
        pl.semaphore_signal(
            barrier, inc=1, device_id={"tp": lax.rem(my_tp + d, heads)}, device_id_type=MESH
        )

    def total_copy(d):
        return pltpu.make_async_remote_copy(
            src_ref=totals.at[0, pl.ds(0, 1)],
            dst_ref=totals.at[d, pl.ds(0, 1)],
            send_sem=tot_send.at[d],
            recv_sem=tot_recv.at[d],
            device_id={"kv": lax.rem(me + d, n)},
            device_id_type=MESH,
        )

    def q_copy(src, dst, side, target):
        return pltpu.make_async_remote_copy(
            src_ref=qbuf.at[src, side],
            dst_ref=qbuf.at[dst, side],
            send_sem=q_send.at[dst, side],
            recv_sem=q_recv.at[dst, side],
            device_id={"kv": target},
            device_id_type=MESH,
        )

    def acc_copies(src, dst, side, target):
        return (
            pltpu.make_async_remote_copy(
                src_ref=acc_out.at[src, side],
                dst_ref=acc_in.at[dst, side],
                send_sem=acc_send.at[src, side],
                recv_sem=acc_recv.at[dst, side],
                device_id={"kv": target},
                device_id_type=MESH,
            ),
            pltpu.make_async_remote_copy(
                src_ref=ml_out.at[src, side, pl.ds(0, 2)],
                dst_ref=ml_in.at[dst, side, pl.ds(0, 2)],
                send_sem=ml_send.at[src, side],
                recv_sem=ml_recv.at[dst, side],
                device_id={"kv": target},
                device_id_type=MESH,
            ),
        )

    def att_copy(d, src_slot, dst_slot):
        return pltpu.make_async_remote_copy(
            src_ref=att.at[src_slot],
            dst_ref=att.at[dst_slot],
            send_sem=att_send.at[d],
            recv_sem=att_recv.at[d],
            device_id={"tp": lax.rem(my_tp + d, heads)},
            device_id_type=MESH,
        )

    def datt_copy(d, src_slot, dst_slot):
        return pltpu.make_async_remote_copy(
            src_ref=datt.at[src_slot],
            dst_ref=datt.at[dst_slot],
            send_sem=datt_send.at[d],
            recv_sem=datt_recv.at[d],
            device_id={"tp": lax.rem(my_tp + d, heads)},
            device_id_type=MESH,
        )

    gain = gain_ref[...]
    rows_at_once = 64

    def norm_rows(x):
        x = x.astype(f32)
        factor = lax.rsqrt(jnp.mean(x * x, axis=-1, keepdims=True) + norm_eps)
        return (x * factor * gain).astype(bf16)

    loads[0].wait()
    for c in loads[2:]:
        c.start()
    for r in range(0, piece, rows_at_once):
        normed[r : r + rows_at_once, :] = norm_rows(tok[r : r + rows_at_once, :])
    drows = norm_rows(dtok_ref[...])
    normed[piece:, :] = jnp.concatenate(
        [drows, jnp.zeros((normed.shape[0] - piece - decs, width), bf16)], axis=0
    )
    loads[1].wait()
    queries = dot(normed[...], wq[...]).astype(bf16)
    q_t = queries[:piece, :].T
    for side in range(2):
        qbuf[0, side] = q_t[:, side * half : (side + 1) * half]
    gate_rows = jnp.broadcast_to(fw_ref[...], (LANES, width))
    gate_in = (
        lax.dot_general(
            normed[...], gate_rows, (((1,), (1,)), ((), ())), preferred_element_type=f32
        )[:, 0:1]
        + fb_ref[0]
    )
    log_gates = jnp.minimum(gate_in, 0.0) - jnp.log1p(jnp.exp(-jnp.abs(gate_in)))
    piece_gates = log_gates[:piece]
    lane = lax.broadcasted_iota(jnp.int32, (piece, LANES), 1)
    hi, mid, lo = three_parts(piece_gates)
    zero = jnp.zeros((), f32)

    def columns(a, b, c, rows):
        at = lax.broadcasted_iota(jnp.int32, (rows, LANES), 1)
        out = jnp.where(at == 0, a.astype(f32), zero)
        out = jnp.where(at == 1, b.astype(f32), out)
        out = jnp.where(at == 2, c.astype(f32), out)
        return out.astype(bf16)

    below = (
        lax.broadcasted_iota(jnp.int32, (piece, piece), 1)
        <= lax.broadcasted_iota(jnp.int32, (piece, piece), 0)
    ).astype(f32)
    running = dot(below.astype(bf16), columns(hi, mid, lo, piece))
    running = running[:, 0:1] + running[:, 1:2] + running[:, 2:3]
    totals[0] = jnp.broadcast_to(running[piece - 1 : piece, :], (8, LANES))

    pl.semaphore_wait(barrier, n - 1 + heads - 1)
    for side, target in ((0, right), (1, left)):
        q_copy(0, 1, side, target).start()
    for d in range(1, n):
        total_copy(d).start()
    for c in range(1, chains):
        o = 1 + c * length
        q_copy(0, o, 0, lax.rem(me + o, n)).start()
        q_copy(0, o, 1, lax.rem(me - o + n, n)).start()

    loads[2].wait()
    key_rows = dot(normed[...], wk[...]).astype(bf16)
    pk_ref[...] = key_rows[:piece]
    kaug[cache:, :depth] = key_rows[:piece]
    loads[3].wait()
    value_rows = dot(normed[...], wv[...]).astype(bf16)
    pv_ref[...] = value_rows[:piece]
    v_t[:depth, cache:] = value_rows[:piece].T
    v_t[depth:, :] = jnp.ones((v_t.shape[0] - depth, v_t.shape[1]), bf16)
    kaug[cache:, depth:] = columns(*three_parts(-running * root), piece)
    at_row = lax.broadcasted_iota(jnp.int32, (LANES, 2 * piece), 0)
    ones_rows[...] = jnp.where(at_row < 3, 1.0, 0.0)[:, :piece].astype(bf16)
    for r in range(0, cache, 512):
        gates = jnp.maximum(cg_ref[:, r : r + 512], NEG) * root
        a, b, c = three_parts(gates)
        at = lax.broadcasted_iota(jnp.int32, (LANES, 512), 0)
        rows = jnp.where(at == 0, a.astype(f32), zero)
        rows = jnp.where(at == 1, b.astype(f32), rows)
        rows = jnp.where(at == 2, c.astype(f32), rows)
        kaug[r : r + 512, depth:] = rows.astype(bf16).T
    loads[4].wait()
    for r in range(0, cache, 512):
        v_t[:depth, r : r + 512] = cv[r : r + 512, :].T
    loads[5].wait()

    dec_rows[0] = queries[piece:, :]
    dec_rows[1] = key_rows[piece:, :]
    dec_rows[2] = value_rows[piece:, :]
    dec_gate[...] = jnp.broadcast_to(log_gates[piece:, :], dec_gate.shape)

    def decode():
        loads[6].wait()
        dec_q = dec_rows[0]
        dec_k = dec_rows[1]
        dec_v = dec_rows[2]
        scores = []
        for b in range(decs):
            s = lax.dot_general(
                dec_q, dk[b], (((1,), (1,)), ((), ())), preferred_element_type=f32
            )
            scores.append(s[b : b + 1])
        gates = jnp.concatenate([dg_ref[b] for b in range(decs)], axis=0)
        cached = jnp.concatenate(scores, axis=0) * scale + gates + dec_gate[0:decs, 0:1]
        slot = lax.broadcasted_iota(jnp.int32, (1, span), 1)
        live = jnp.concatenate(
            [jnp.where(slot < dl_ref[b], 1.0, 0.0) for b in range(decs)], axis=0
        )
        cached = jnp.where(live > 0.5, cached, -jnp.inf)
        own_score = (
            jnp.sum(dec_q.astype(f32) * dec_k.astype(f32), axis=-1, keepdims=True)[:decs] * scale
        )
        top = jnp.maximum(jnp.max(cached, axis=-1, keepdims=True), own_score)
        cached_exp = jnp.exp(cached - top)
        own_exp = jnp.exp(own_score - top)
        whole = jnp.sum(cached_exp, axis=-1, keepdims=True) + own_exp
        weights = (cached_exp / whole).astype(bf16)
        own_weight = (own_exp / whole).astype(bf16).astype(f32)
        weights = jnp.concatenate(
            [weights, jnp.zeros((dec_q.shape[0] - decs, span), bf16)], axis=0
        )
        loads[7].wait()
        mixed = [dot(weights, dv[b])[b : b + 1] for b in range(decs)]
        mixed = jnp.concatenate(mixed, axis=0) + own_weight * dec_v[:decs].astype(f32)
        datt[0] = jnp.concatenate(
            [mixed, jnp.zeros((dec_q.shape[0] - decs, depth), f32)], axis=0
        ).astype(bf16)
        for d in range(1, heads):
            datt_copy(d, 0, d).start()

    chunks = [(cache, cache + piece)] + [
        (k, k + KEY_CHUNK) for k in range(0, cache, KEY_CHUNK)
    ]
    lane_row = lax.broadcasted_iota(jnp.int32, (1, piece), 1)

    def local_terms(o, offset):
        block_a = lax.rem(me - o + n, n)
        block_b = lax.rem(me + o, n)
        slot_o = lax.rem(o, n)
        q_block = jnp.concatenate([qbuf[slot_o, 0], qbuf[slot_o, 1]], axis=1)
        q_block = jnp.concatenate([q_block, ones_rows[...]], axis=0)
        query_order = jnp.where(lane_row < half, block_a, block_b) * piece + lane_row
        s = dot(kaug[chunks[0][0] : chunks[0][1], :], q_block)
        terms = []
        for i, (k0, k1) in enumerate(chunks):
            if i == 0:
                key_order = me * piece + lax.broadcasted_iota(jnp.int32, (piece, 1), 0)
                s = jnp.where(key_order <= query_order, s, NEG)
            top_i = row_max(s)
            if i + 1 < len(chunks):
                s_next = dot(kaug[chunks[i + 1][0] : chunks[i + 1][1], :], q_block)
            weights_i = jnp.exp2((s - top_i) * c2).astype(bf16)
            sums = dot(v_t[:, k0:k1], weights_i)
            terms.append((sums, top_i - offset * root if i == 0 else top_i))
            s = s_next
        top_all = functools.reduce(jnp.maximum, [t for _, t in terms])
        total = None
        for sums, t in terms:
            part = sums * jnp.exp2((t - top_all) * c2)
            total = part if total is None else total + part
        return total[:depth], top_all, total[depth : depth + 1]

    def ml_rows(m, l):
        return jnp.concatenate([m, l, jnp.zeros((6, m.shape[1]), f32)], axis=0)

    def merge(acc_a, m_a, l_a, acc_b, m_b, l_b):
        m = jnp.maximum(m_a, m_b)
        f_a = jnp.exp2((m_a - m) * c2)
        f_b = jnp.exp2((m_b - m) * c2)
        return acc_a * f_a + acc_b * f_b, m, l_a * f_a + l_b * f_b

    for d in range(1, n):
        total_copy(d).wait_recv()
    offset = jnp.zeros((1, LANES), f32)
    for d in range(1, n):
        offset = offset + jnp.where(d <= me, totals[d][0:1, :], 0.0)
    offset = jnp.concatenate([offset] * (piece // LANES), axis=1)

    skew = 2 if chains > 1 else 0
    paired = length - skew if chains > 1 else 0

    def order(u):
        if chains == 1:
            return jnp.where(u == 0, 1, jnp.where(u == 1, n, u))
        k = u - 1 - skew
        middle = jnp.where(
            lax.rem(k, 2) == 0, 1 + skew + k // 2, 1 + length + k // 2
        )
        o = jnp.where(u < 1 + skew, u, jnp.where(k < 2 * paired, middle, u))
        return jnp.where(u == 0, 1, jnp.where(u == 1, n, o))

    def unit(u, carry):
        o = order(u)
        starts = lax.rem(o, length) == 1
        ends = lax.rem(o, length) == 0

        @pl.when(o < n)
        def _():
            for side in range(2):
                q_copy(0, o, side, right).wait_recv()

        @pl.when(jnp.logical_and(jnp.logical_not(ends), o < n - 1))
        def _():
            for side, target in ((0, right), (1, left)):
                q_copy(o, o + 1, side, target).start()

        @pl.when(u == 2)
        def _():
            decode()

        acc, m, l = local_terms(o, offset)
        unit_acc[...] = acc
        unit_ml[...] = ml_rows(m, l)

        @pl.when(o == n)
        def _():
            own_acc[...] = unit_acc[...]
            own_ml[...] = unit_ml[...]

        @pl.when(o < n)
        def _():
            @pl.when(starts)
            def _():
                for side in range(2):
                    acc_in[o, side] = jnp.zeros((depth, half), bf16)
                    ml_in[o, side] = jnp.where(
                        lax.broadcasted_iota(jnp.int32, (8, half), 0) == 0, NEG, 0.0
                    )

            @pl.when(jnp.logical_not(starts))
            def _():
                for side in range(2):
                    for c in acc_copies(0, o, side, right):
                        c.wait_recv()

            for side in range(2):
                at = slice(side * half, (side + 1) * half)
                ml = ml_in[o, side]
                a, mm, ll = merge(
                    unit_acc[:, at],
                    unit_ml[0:1, at],
                    unit_ml[1:2, at],
                    acc_in[o, side].astype(f32),
                    ml[0:1],
                    ml[1:2],
                )
                acc_out[o, side] = a.astype(bf16)
                ml_out[o, side] = ml_rows(mm, ll)
            goes = jnp.where(ends, o, 1)
            dst = jnp.where(ends, n + o // length, o + 1)
            for c in acc_copies(o, dst, 0, lax.rem(me + jnp.where(ends, n - goes, 1), n)):
                c.start()
            for c in acc_copies(o, dst, 1, lax.rem(me + jnp.where(ends, goes, n - 1), n)):
                c.start()

        return carry

    lax.fori_loop(0, n, unit, 0)

    halves = []
    for side in range(2):
        at = slice(side * half, (side + 1) * half)
        state = (own_acc[:, at], own_ml[0:1, at], own_ml[1:2, at])
        for slot_i in [n + c for c in range(1, chains)] + [n]:
            for c in acc_copies(0, slot_i, side, right):
                c.wait_recv()
            ml = ml_in[slot_i, side]
            state = merge(*state, acc_in[slot_i, side].astype(f32), ml[0:1], ml[1:2])
        halves.append((state[0] / state[2]).astype(bf16))
    att[0] = jnp.concatenate(halves, axis=1).T
    for d in range(1, heads):
        att_copy(d, 0, d).start()

    def weight_of(d):
        head = lax.rem(my_tp - d + heads, heads)
        return ow[pl.ds(pl.multiple_of(head * depth, depth), depth), :]

    loads[8].wait()
    dec_sum = dot(datt[0], weight_of(0))
    for d in range(1, heads):
        datt_copy(d, 0, d).wait_recv()
        dec_sum = dec_sum + dot(datt[d], weight_of(d))
    do_ref[...] = dec_sum[:decs].astype(bf16)
    out = dot(att[0], weight_of(0))
    for d in range(1, heads):
        att_copy(d, 0, d).wait_recv()
        out = out + dot(att[d], weight_of(d))
    po_ref[...] = out.astype(bf16)

    for d in range(1, n):
        total_copy(d).wait_send()
    for d in range(1, heads):
        att_copy(d, 0, d).wait_send()
        datt_copy(d, 0, d).wait_send()

    def sent(o, carry):
        for side in range(2):
            q_copy(0, o, side, right).wait_send()
            for c in acc_copies(o, n, side, right):
                c.wait_send()
        return carry

    lax.fori_loop(1, n, sent, 0)


def hand_over(*refs):
    for src, dst in zip(refs[:4], refs[4:]):
        dst[...] = src[...]


def shards(
    piece_tokens,
    dec_tokens,
    norm_gain,
    query_weight,
    key_weight,
    value_weight,
    forget_weight,
    forget_bias,
    out_weight,
    cache_keys,
    cache_values,
    cache_gates,
    dec_keys,
    dec_values,
    dec_gates,
    dec_lengths,
):
    n = lax.axis_size("kv")
    heads = lax.axis_size("tp")
    piece, width = piece_tokens.shape
    decs, span = dec_tokens.shape[0], dec_keys.shape[1]
    depth = query_weight.shape[1]
    cache = cache_keys.shape[0]
    out_columns = out_weight.shape[1]
    half = piece // 2
    chains = 2
    rows = piece + 16
    vmem = pl.BlockSpec(memory_space=pltpu.VMEM)
    hbm = pl.BlockSpec(memory_space=pl.ANY)
    dma = pltpu.SemaphoreType.DMA
    slots = n + chains
    smem = pl.BlockSpec(memory_space=pltpu.SMEM)
    results = pl.pallas_call(
        functools.partial(kernel, chains=chains),
        out_shape=(
            jax.ShapeDtypeStruct((piece, out_columns), bf16),
            jax.ShapeDtypeStruct((decs, out_columns), bf16),
            jax.ShapeDtypeStruct((piece, depth), bf16),
            jax.ShapeDtypeStruct((piece, depth), bf16),
        ),
        in_specs=[hbm, vmem, vmem, hbm, hbm, hbm, vmem, smem, hbm, hbm, hbm, vmem, hbm, hbm, vmem, smem],
        out_specs=(vmem, vmem, vmem, vmem),
        scratch_shapes=[
            pltpu.VMEM((piece, width), bf16),
            pltpu.VMEM((width, depth), bf16),
            pltpu.VMEM((width, depth), bf16),
            pltpu.VMEM((width, depth), bf16),
            pltpu.VMEM(out_weight.shape, bf16),
            pltpu.VMEM((cache, depth), bf16),
            pltpu.VMEM(dec_keys.shape, bf16),
            pltpu.VMEM(dec_values.shape, bf16),
            pltpu.VMEM((rows, width), bf16),
            pltpu.VMEM((cache + piece, depth + LANES), bf16),
            pltpu.VMEM((depth + 16, cache + piece), bf16),
            pltpu.VMEM((LANES, piece), bf16),
            pltpu.VMEM((n, 2, depth, half), bf16),
            pltpu.VMEM((slots, 2, depth, half), bf16),
            pltpu.VMEM((slots, 2, 8, half), f32),
            pltpu.VMEM((n, 2, depth, half), bf16),
            pltpu.VMEM((n, 2, 8, half), f32),
            pltpu.VMEM((depth, piece), f32),
            pltpu.VMEM((8, piece), f32),
            pltpu.VMEM((depth, piece), f32),
            pltpu.VMEM((8, piece), f32),
            pltpu.VMEM((n, 8, LANES), f32),
            pltpu.VMEM((heads, piece, depth), bf16),
            pltpu.VMEM((heads, 16, depth), bf16),
            pltpu.VMEM((3, 16, depth), bf16),
            pltpu.VMEM((16, LANES), f32),
            dma((9,)),
            dma((n, 2)),
            dma((n, 2)),
            dma((n, 2)),
            dma((slots, 2)),
            dma((n, 2)),
            dma((slots, 2)),
            dma((n,)),
            dma((n,)),
            dma((heads,)),
            dma((heads,)),
            dma((heads,)),
            dma((heads,)),
        ],
        compiler_params=pltpu.CompilerParams(
            collective_id=0, has_side_effects=True, vmem_limit_bytes=60 * 2**20
        ),
    )(
        piece_tokens,
        dec_tokens,
        norm_gain.reshape(1, width),
        query_weight,
        key_weight,
        value_weight,
        forget_weight.reshape(1, width),
        forget_bias,
        out_weight,
        cache_keys,
        cache_values,
        cache_gates,
        dec_keys,
        dec_values,
        dec_gates,
        dec_lengths,
    )
    return pl.pallas_call(
        hand_over,
        out_shape=tuple(jax.ShapeDtypeStruct(r.shape, r.dtype) for r in results),
        in_specs=[vmem] * 4,
        out_specs=(vmem,) * 4,
    )(*results)


def solution(mesh):
    return jax.shard_map(
        shards,
        mesh=mesh,
        in_specs=(
            P(("grp", "kv"), None),
            P(("grp", "kv"), None),
            P(),
            P(None, "tp"),
            P(None, "tp"),
            P(None, "tp"),
            P(None, "tp"),
            P("tp"),
            P(None, "tp"),
            P(("grp", "kv"), "tp"),
            P(("grp", "kv"), "tp"),
            P("tp", ("grp", "kv")),
            P(("grp", "kv"), None, "tp"),
            P(("grp", "kv"), None, "tp"),
            P(("grp", "kv"), "tp", None),
            P(("grp", "kv")),
        ),
        out_specs=(
            P(("grp", "kv"), "tp"),
            P(("grp", "kv"), "tp"),
            P(("grp", "kv"), "tp"),
            P(("grp", "kv"), "tp"),
        ),
        check_vma=False,
    )
```

```python
import functools
import math

import jax
import jax.numpy as jnp
from jax import lax
from jax.experimental import pallas as pl
from jax.experimental.pallas import tpu as pltpu
from jax.sharding import PartitionSpec as P

norm_eps = 1e-05
bf16 = jnp.bfloat16
f32 = jnp.float32
MESH = pl.DeviceIdType.MESH
NEG = -1e30
LANES = 128
KEY_CHUNK = 2048


def dot(a, b):
    return jnp.dot(a, b, preferred_element_type=f32)


def three_parts(x):
    high = x.astype(bf16)
    rest = x - high.astype(f32)
    middle = rest.astype(bf16)
    low = (rest - middle.astype(f32)).astype(bf16)
    return high, middle, low


def row_max(x, rows=64):
    n = x.shape[0]
    if n > rows:
        x = jnp.max(x.reshape(n // rows, rows, x.shape[1]), axis=0)
    return jnp.max(x, axis=0, keepdims=True)


def kernel(
    tok_hbm,
    dtok_ref,
    gain_ref,
    wq_hbm,
    wk_hbm,
    wv_hbm,
    fw_ref,
    fb_ref,
    ow_hbm,
    ck_hbm,
    cv_hbm,
    cg_ref,
    dk_hbm,
    dv_hbm,
    dg_ref,
    dl_ref,
    po_ref,
    do_ref,
    pk_ref,
    pv_ref,
    tok,
    wq,
    wk,
    wv,
    ow,
    cv,
    dk,
    dv,
    normed,
    kaug,
    v_t,
    ones_rows,
    qbuf,
    acc_in,
    ml_in,
    acc_out,
    ml_out,
    unit_acc,
    unit_ml,
    own_acc,
    own_ml,
    totals,
    att,
    datt,
    dec_rows,
    dec_gate,
    local_sem,
    q_send,
    q_recv,
    acc_send,
    acc_recv,
    ml_send,
    ml_recv,
    tot_send,
    tot_recv,
    att_send,
    att_recv,
    datt_send,
    datt_recv,
):
    n = lax.axis_size("kv")
    heads = lax.axis_size("tp")
    me = lax.axis_index("kv")
    my_tp = lax.axis_index("tp")
    right = lax.rem(me + 1, n)
    left = lax.rem(me + n - 1, n)
    piece, width = tok.shape
    half = piece // 2
    depth = wq.shape[1]
    cache = cv.shape[0]
    decs, span = dk.shape[0], dk.shape[1]
    split = n // 2
    scale = depth ** (-0.5)
    root = depth**0.5
    c2 = scale * math.log2(math.e)

    def load(i, src, dst):
        return pltpu.make_async_copy(src, dst, local_sem.at[i])

    loads = [
        load(0, tok_hbm, tok),
        load(1, wq_hbm, wq),
        load(2, wk_hbm, wk),
        load(3, wv_hbm, wv),
        load(4, cv_hbm, cv),
        load(5, ck_hbm, kaug.at[pl.ds(0, cache), pl.ds(0, depth)]),
        load(6, dk_hbm, dk),
        load(7, dv_hbm, dv),
        load(8, ow_hbm, ow),
    ]
    loads[0].start()
    loads[1].start()
    barrier = pltpu.get_barrier_semaphore()
    for d in range(1, n):
        pl.semaphore_signal(
            barrier, inc=1, device_id={"kv": lax.rem(me + d, n)}, device_id_type=MESH
        )
    for d in range(1, heads):
        pl.semaphore_signal(
            barrier, inc=1, device_id={"tp": lax.rem(my_tp + d, heads)}, device_id_type=MESH
        )

    def total_copy(d):
        return pltpu.make_async_remote_copy(
            src_ref=totals.at[0, pl.ds(0, 1)],
            dst_ref=totals.at[d, pl.ds(0, 1)],
            send_sem=tot_send.at[d],
            recv_sem=tot_recv.at[d],
            device_id={"kv": lax.rem(me + d, n)},
            device_id_type=MESH,
        )

    def q_copy(src, dst, side, target):
        return pltpu.make_async_remote_copy(
            src_ref=qbuf.at[src, side],
            dst_ref=qbuf.at[dst, side],
            send_sem=q_send.at[dst, side],
            recv_sem=q_recv.at[dst, side],
            device_id={"kv": target},
            device_id_type=MESH,
        )

    def acc_copies(src, dst, side, target):
        return (
            pltpu.make_async_remote_copy(
                src_ref=acc_out.at[src, side],
                dst_ref=acc_in.at[dst, side],
                send_sem=acc_send.at[src, side],
                recv_sem=acc_recv.at[dst, side],
                device_id={"kv": target},
                device_id_type=MESH,
            ),
            pltpu.make_async_remote_copy(
                src_ref=ml_out.at[src, side, pl.ds(0, 2)],
                dst_ref=ml_in.at[dst, side, pl.ds(0, 2)],
                send_sem=ml_send.at[src, side],
                recv_sem=ml_recv.at[dst, side],
                device_id={"kv": target},
                device_id_type=MESH,
            ),
        )

    def att_copy(d, src_slot, dst_slot):
        return pltpu.make_async_remote_copy(
            src_ref=att.at[src_slot],
            dst_ref=att.at[dst_slot],
            send_sem=att_send.at[d],
            recv_sem=att_recv.at[d],
            device_id={"tp": lax.rem(my_tp + d, heads)},
            device_id_type=MESH,
        )

    def datt_copy(d, src_slot, dst_slot):
        return pltpu.make_async_remote_copy(
            src_ref=datt.at[src_slot],
            dst_ref=datt.at[dst_slot],
            send_sem=datt_send.at[d],
            recv_sem=datt_recv.at[d],
            device_id={"tp": lax.rem(my_tp + d, heads)},
            device_id_type=MESH,
        )

    gain = gain_ref[...]
    rows_at_once = 64

    def norm_rows(x):
        x = x.astype(f32)
        factor = lax.rsqrt(jnp.mean(x * x, axis=-1, keepdims=True) + norm_eps)
        return (x * factor * gain).astype(bf16)

    loads[0].wait()
    for c in loads[2:]:
        c.start()
    for r in range(0, piece, rows_at_once):
        normed[r : r + rows_at_once, :] = norm_rows(tok[r : r + rows_at_once, :])
    drows = norm_rows(dtok_ref[...])
    normed[piece:, :] = jnp.concatenate(
        [drows, jnp.zeros((normed.shape[0] - piece - decs, width), bf16)], axis=0
    )
    loads[1].wait()
    queries = dot(normed[...], wq[...]).astype(bf16)
    q_t = queries[:piece, :].T
    for side in range(2):
        qbuf[0, side] = q_t[:, side * half : (side + 1) * half]
    gate_rows = jnp.broadcast_to(fw_ref[...], (LANES, width))
    gate_in = (
        lax.dot_general(
            normed[...], gate_rows, (((1,), (1,)), ((), ())), preferred_element_type=f32
        )[:, 0:1]
        + fb_ref[0]
    )
    log_gates = jnp.minimum(gate_in, 0.0) - jnp.log1p(jnp.exp(-jnp.abs(gate_in)))
    piece_gates = log_gates[:piece]
    lane = lax.broadcasted_iota(jnp.int32, (piece, LANES), 1)
    hi, mid, lo = three_parts(piece_gates)
    zero = jnp.zeros((), f32)

    def columns(a, b, c, rows):
        at = lax.broadcasted_iota(jnp.int32, (rows, LANES), 1)
        out = jnp.where(at == 0, a.astype(f32), zero)
        out = jnp.where(at == 1, b.astype(f32), out)
        out = jnp.where(at == 2, c.astype(f32), out)
        return out.astype(bf16)

    below = (
        lax.broadcasted_iota(jnp.int32, (piece, piece), 1)
        <= lax.broadcasted_iota(jnp.int32, (piece, piece), 0)
    ).astype(f32)
    running = dot(below.astype(bf16), columns(hi, mid, lo, piece))
    running = running[:, 0:1] + running[:, 1:2] + running[:, 2:3]
    totals[0] = jnp.broadcast_to(running[piece - 1 : piece, :], (8, LANES))

    pl.semaphore_wait(barrier, n - 1 + heads - 1)
    for side, target in ((0, right), (1, left)):
        q_copy(0, 1, side, target).start()
    for d in range(1, n):
        total_copy(d).start()
    second = split + 1
    q_copy(0, second, 0, lax.rem(me + second, n)).start()
    q_copy(0, second, 1, lax.rem(me - second + n, n)).start()

    loads[2].wait()
    key_rows = dot(normed[...], wk[...]).astype(bf16)
    pk_ref[...] = key_rows[:piece]
    kaug[cache:, :depth] = key_rows[:piece]
    loads[3].wait()
    value_rows = dot(normed[...], wv[...]).astype(bf16)
    pv_ref[...] = value_rows[:piece]
    v_t[:depth, cache:] = value_rows[:piece].T
    v_t[depth:, :] = jnp.ones((v_t.shape[0] - depth, v_t.shape[1]), bf16)
    kaug[cache:, depth:] = columns(*three_parts(-running * root), piece)
    at_row = lax.broadcasted_iota(jnp.int32, (LANES, 2 * piece), 0)
    ones_rows[...] = jnp.where(at_row < 3, 1.0, 0.0)[:, :piece].astype(bf16)
    for r in range(0, cache, 512):
        gates = jnp.maximum(cg_ref[:, r : r + 512], NEG) * root
        a, b, c = three_parts(gates)
        at = lax.broadcasted_iota(jnp.int32, (LANES, 512), 0)
        rows = jnp.where(at == 0, a.astype(f32), zero)
        rows = jnp.where(at == 1, b.astype(f32), rows)
        rows = jnp.where(at == 2, c.astype(f32), rows)
        kaug[r : r + 512, depth:] = rows.astype(bf16).T
    loads[4].wait()
    for r in range(0, cache, 512):
        v_t[:depth, r : r + 512] = cv[r : r + 512, :].T
    loads[5].wait()

    dec_rows[0] = queries[piece:, :]
    dec_rows[1] = key_rows[piece:, :]
    dec_rows[2] = value_rows[piece:, :]
    dec_gate[...] = jnp.broadcast_to(log_gates[piece:, :], dec_gate.shape)

    def decode():
        loads[6].wait()
        dec_q = dec_rows[0]
        dec_k = dec_rows[1]
        dec_v = dec_rows[2]
        scores = []
        for b in range(decs):
            s = lax.dot_general(
                dec_q, dk[b], (((1,), (1,)), ((), ())), preferred_element_type=f32
            )
            scores.append(s[b : b + 1])
        gates = jnp.concatenate([dg_ref[b] for b in range(decs)], axis=0)
        cached = jnp.concatenate(scores, axis=0) * scale + gates + dec_gate[0:decs, 0:1]
        slot = lax.broadcasted_iota(jnp.int32, (1, span), 1)
        live = jnp.concatenate(
            [jnp.where(slot < dl_ref[b], 1.0, 0.0) for b in range(decs)], axis=0
        )
        cached = jnp.where(live > 0.5, cached, -jnp.inf)
        own_score = (
            jnp.sum(dec_q.astype(f32) * dec_k.astype(f32), axis=-1, keepdims=True)[:decs] * scale
        )
        top = jnp.maximum(jnp.max(cached, axis=-1, keepdims=True), own_score)
        cached_exp = jnp.exp(cached - top)
        own_exp = jnp.exp(own_score - top)
        whole = jnp.sum(cached_exp, axis=-1, keepdims=True) + own_exp
        weights = (cached_exp / whole).astype(bf16)
        own_weight = (own_exp / whole).astype(bf16).astype(f32)
        weights = jnp.concatenate(
            [weights, jnp.zeros((dec_q.shape[0] - decs, span), bf16)], axis=0
        )
        loads[7].wait()
        mixed = [dot(weights, dv[b])[b : b + 1] for b in range(decs)]
        mixed = jnp.concatenate(mixed, axis=0) + own_weight * dec_v[:decs].astype(f32)
        datt[0] = jnp.concatenate(
            [mixed, jnp.zeros((dec_q.shape[0] - decs, depth), f32)], axis=0
        ).astype(bf16)
        for d in range(1, heads):
            datt_copy(d, 0, d).start()

    chunks = [(cache, cache + piece)] + [
        (k, k + KEY_CHUNK) for k in range(0, cache, KEY_CHUNK)
    ]
    lane_row = lax.broadcasted_iota(jnp.int32, (1, piece), 1)

    def local_terms(offsets, shift):
        steps = []
        for which, o in enumerate(offsets):
            block_a = lax.rem(me - o + n, n)
            block_b = lax.rem(me + o, n)
            slot_o = lax.rem(o, n)
            q_block = jnp.concatenate([qbuf[slot_o, 0], qbuf[slot_o, 1]], axis=1)
            q_block = jnp.concatenate([q_block, ones_rows[...]], axis=0)
            query_order = jnp.where(lane_row < half, block_a, block_b) * piece + lane_row
            steps += [(which, q_block, query_order, k0, k1) for k0, k1 in chunks]
        terms = [[] for _ in offsets]
        s = dot(kaug[steps[0][3] : steps[0][4], :], steps[0][1])
        for i, (which, q_block, query_order, k0, k1) in enumerate(steps):
            if k0 == cache:
                key_order = me * piece + lax.broadcasted_iota(jnp.int32, (piece, 1), 0)
                s = jnp.where(key_order <= query_order, s, NEG)
            top_i = row_max(s)
            if i + 1 < len(steps):
                s_next = dot(kaug[steps[i + 1][3] : steps[i + 1][4], :], steps[i + 1][1])
            weights_i = jnp.exp2((s - top_i) * c2).astype(bf16)
            sums = dot(v_t[:, k0:k1], weights_i)
            terms[which].append((sums, top_i - shift * root if k0 == cache else top_i))
            s = s_next
        results = []
        for mine in terms:
            top_all = functools.reduce(jnp.maximum, [t for _, t in mine])
            total = None
            for sums, t in mine:
                part = sums * jnp.exp2((t - top_all) * c2)
                total = part if total is None else total + part
            results.append((total[:depth], top_all, total[depth : depth + 1]))
        return results

    def ml_rows(m, l):
        return jnp.concatenate([m, l, jnp.zeros((6, m.shape[1]), f32)], axis=0)

    def merge(acc_a, m_a, l_a, acc_b, m_b, l_b):
        m = jnp.maximum(m_a, m_b)
        f_a = jnp.exp2((m_a - m) * c2)
        f_b = jnp.exp2((m_b - m) * c2)
        return acc_a * f_a + acc_b * f_b, m, l_a * f_a + l_b * f_b

    for d in range(1, n):
        total_copy(d).wait_recv()
    offset = jnp.zeros((1, LANES), f32)
    for d in range(1, n):
        offset = offset + jnp.where(d <= me, totals[d][0:1, :], 0.0)
    offset = jnp.concatenate([offset] * (piece // LANES), axis=1)

    def arrived(o):
        for side in range(2):
            q_copy(0, o, side, right).wait_recv()

    def forward(o):
        for side, target in ((0, right), (1, left)):
            q_copy(o, o + 1, side, target).start()

    def settle(which, o, starts, ends):
        @pl.when(starts)
        def _():
            for side in range(2):
                acc_in[o, side] = jnp.zeros((depth, half), bf16)
                ml_in[o, side] = jnp.where(
                    lax.broadcasted_iota(jnp.int32, (8, half), 0) == 0, NEG, 0.0
                )

        @pl.when(jnp.logical_not(starts))
        def _():
            for side in range(2):
                for c in acc_copies(0, o, side, right):
                    c.wait_recv()

        away = jnp.where(ends, o, n - 1)
        dst = jnp.where(ends, n + 1, o + 1)
        targets = (lax.rem(me + n - jnp.where(ends, o, n - 1), n), lax.rem(me + away, n))
        for side in range(2):
            at = slice(side * half, (side + 1) * half)
            ml = ml_in[o, side]
            a, mm, ll = merge(
                unit_acc[which, :, at],
                unit_ml[which, 0:1, at],
                unit_ml[which, 1:2, at],
                acc_in[o, side].astype(f32),
                ml[0:1],
                ml[1:2],
            )
            acc_out[o, side] = a.astype(bf16)
            ml_out[o, side] = ml_rows(mm, ll)
        for side in range(2):
            for c in acc_copies(o, dst, side, targets[side]):
                c.start()

    def pair(it, carry):
        first = it + 1
        other = jnp.where(it == 0, n, split + it)
        arrived(first)

        @pl.when(first < split)
        def _():
            forward(first)

        @pl.when(it == 1)
        def _():
            decode()

        @pl.when(it > 0)
        def _():
            arrived(other)

            @pl.when(other < n - 1)
            def _():
                forward(other)

        for which, (acc, m, l) in enumerate(local_terms((first, other), offset)):
            unit_acc[which] = acc
            unit_ml[which] = ml_rows(m, l)

        settle(0, first, it == 0, first == split)

        @pl.when(it == 0)
        def _():
            own_acc[...] = unit_acc[1]
            own_ml[...] = unit_ml[1]

        @pl.when(it > 0)
        def _():
            settle(1, other, it == 1, other == n)

        return carry

    lax.fori_loop(0, split, pair, 0)

    halves = []
    for side in range(2):
        at = slice(side * half, (side + 1) * half)
        state = (own_acc[:, at], own_ml[0:1, at], own_ml[1:2, at])
        for slot_i in (n + 1, n):
            for c in acc_copies(0, slot_i, side, right):
                c.wait_recv()
            ml = ml_in[slot_i, side]
            state = merge(*state, acc_in[slot_i, side].astype(f32), ml[0:1], ml[1:2])
        halves.append((state[0] / state[2]).astype(bf16))
    att[0] = jnp.concatenate(halves, axis=1).T
    for d in range(1, heads):
        att_copy(d, 0, d).start()

    def weight_of(d):
        head = lax.rem(my_tp - d + heads, heads)
        return ow[pl.ds(pl.multiple_of(head * depth, depth), depth), :]

    loads[8].wait()
    dec_sum = dot(datt[0], weight_of(0))
    for d in range(1, heads):
        datt_copy(d, 0, d).wait_recv()
        dec_sum = dec_sum + dot(datt[d], weight_of(d))
    do_ref[...] = dec_sum[:decs].astype(bf16)
    out = dot(att[0], weight_of(0))
    for d in range(1, heads):
        att_copy(d, 0, d).wait_recv()
        out = out + dot(att[d], weight_of(d))
    po_ref[...] = out.astype(bf16)

    for d in range(1, n):
        total_copy(d).wait_send()
    for d in range(1, heads):
        att_copy(d, 0, d).wait_send()
        datt_copy(d, 0, d).wait_send()

    def sent(o, carry):
        for side in range(2):
            q_copy(0, o, side, right).wait_send()
            for c in acc_copies(o, n, side, right):
                c.wait_send()
        return carry

    lax.fori_loop(1, n, sent, 0)


def hand_over(*refs):
    for src, dst in zip(refs[:4], refs[4:]):
        dst[...] = src[...]


def shards(
    piece_tokens,
    dec_tokens,
    norm_gain,
    query_weight,
    key_weight,
    value_weight,
    forget_weight,
    forget_bias,
    out_weight,
    cache_keys,
    cache_values,
    cache_gates,
    dec_keys,
    dec_values,
    dec_gates,
    dec_lengths,
):
    n = lax.axis_size("kv")
    heads = lax.axis_size("tp")
    piece, width = piece_tokens.shape
    decs, span = dec_tokens.shape[0], dec_keys.shape[1]
    depth = query_weight.shape[1]
    cache = cache_keys.shape[0]
    out_columns = out_weight.shape[1]
    half = piece // 2
    rows = piece + 16
    vmem = pl.BlockSpec(memory_space=pltpu.VMEM)
    hbm = pl.BlockSpec(memory_space=pl.ANY)
    dma = pltpu.SemaphoreType.DMA
    slots = n + 2
    smem = pl.BlockSpec(memory_space=pltpu.SMEM)
    results = pl.pallas_call(
        kernel,
        out_shape=(
            jax.ShapeDtypeStruct((piece, out_columns), bf16),
            jax.ShapeDtypeStruct((decs, out_columns), bf16),
            jax.ShapeDtypeStruct((piece, depth), bf16),
            jax.ShapeDtypeStruct((piece, depth), bf16),
        ),
        in_specs=[hbm, vmem, vmem, hbm, hbm, hbm, vmem, smem, hbm, hbm, hbm, vmem, hbm, hbm, vmem, smem],
        out_specs=(vmem, vmem, vmem, vmem),
        scratch_shapes=[
            pltpu.VMEM((piece, width), bf16),
            pltpu.VMEM((width, depth), bf16),
            pltpu.VMEM((width, depth), bf16),
            pltpu.VMEM((width, depth), bf16),
            pltpu.VMEM(out_weight.shape, bf16),
            pltpu.VMEM((cache, depth), bf16),
            pltpu.VMEM(dec_keys.shape, bf16),
            pltpu.VMEM(dec_values.shape, bf16),
            pltpu.VMEM((rows, width), bf16),
            pltpu.VMEM((cache + piece, depth + LANES), bf16),
            pltpu.VMEM((depth + 16, cache + piece), bf16),
            pltpu.VMEM((LANES, piece), bf16),
            pltpu.VMEM((n, 2, depth, half), bf16),
            pltpu.VMEM((slots, 2, depth, half), bf16),
            pltpu.VMEM((slots, 2, 8, half), f32),
            pltpu.VMEM((n, 2, depth, half), bf16),
            pltpu.VMEM((n, 2, 8, half), f32),
            pltpu.VMEM((2, depth, piece), f32),
            pltpu.VMEM((2, 8, piece), f32),
            pltpu.VMEM((depth, piece), f32),
            pltpu.VMEM((8, piece), f32),
            pltpu.VMEM((n, 8, LANES), f32),
            pltpu.VMEM((heads, piece, depth), bf16),
            pltpu.VMEM((heads, 16, depth), bf16),
            pltpu.VMEM((3, 16, depth), bf16),
            pltpu.VMEM((16, LANES), f32),
            dma((9,)),
            dma((n, 2)),
            dma((n, 2)),
            dma((n, 2)),
            dma((slots, 2)),
            dma((n, 2)),
            dma((slots, 2)),
            dma((n,)),
            dma((n,)),
            dma((heads,)),
            dma((heads,)),
            dma((heads,)),
            dma((heads,)),
        ],
        compiler_params=pltpu.CompilerParams(
            collective_id=0, has_side_effects=True, vmem_limit_bytes=60 * 2**20
        ),
    )(
        piece_tokens,
        dec_tokens,
        norm_gain.reshape(1, width),
        query_weight,
        key_weight,
        value_weight,
        forget_weight.reshape(1, width),
        forget_bias,
        out_weight,
        cache_keys,
        cache_values,
        cache_gates,
        dec_keys,
        dec_values,
        dec_gates,
        dec_lengths,
    )
    return pl.pallas_call(
        hand_over,
        out_shape=tuple(jax.ShapeDtypeStruct(r.shape, r.dtype) for r in results),
        in_specs=[vmem] * 4,
        out_specs=(vmem,) * 4,
    )(*results)


def solution(mesh):
    return jax.shard_map(
        shards,
        mesh=mesh,
        in_specs=(
            P(("grp", "kv"), None),
            P(("grp", "kv"), None),
            P(),
            P(None, "tp"),
            P(None, "tp"),
            P(None, "tp"),
            P(None, "tp"),
            P("tp"),
            P(None, "tp"),
            P(("grp", "kv"), "tp"),
            P(("grp", "kv"), "tp"),
            P("tp", ("grp", "kv")),
            P(("grp", "kv"), None, "tp"),
            P(("grp", "kv"), None, "tp"),
            P(("grp", "kv"), "tp", None),
            P(("grp", "kv")),
        ),
        out_specs=(
            P(("grp", "kv"), "tp"),
            P(("grp", "kv"), "tp"),
            P(("grp", "kv"), "tp"),
            P(("grp", "kv"), "tp"),
        ),
        check_vma=False,
    )
```
